32 devices in a mesh: sp: 8 (over z, y), tp: 4 (over x, core).
Axes of the slice: x: 2, y: 2, z: 4, core: 2. Of those that a mesh axis runs over, the one named last changes fastest.
Arguments:
- layer_input: bfloat16 [8, 1024, 2048], P(None, ('sp', 'tp')), may hold values from -6 to 6
- input_gain: float32 [2048], replicated, may hold values from 0.5 to 1.5
- narrowing_matrix: bfloat16 [2048, 512], replicated, may hold values from -0.125 to 0.125
- rotary_down: bfloat16 [2048, 64], replicated, may hold values from -0.125 to 0.125
- summary_scaling: float32 [512], replicated, may hold values from 0.5 to 1.5
- lookup_widening: bfloat16 [512, 16, 128], P('tp'), may hold values from -0.25 to 0.25
- payload_widening: bfloat16 [512, 16, 128], P('tp'), may hold values from -0.25 to 0.25
- query_nope: bfloat16 [8, 16, 128], P('sp', 'tp'), may hold values from -6 to 6
- query_rotary: bfloat16 [8, 16, 64], P('sp', 'tp'), may hold values from -6 to 6
Outputs:
- stored_summaries: bfloat16 [8, 1024, 512], P('sp', None, 'tp')
- rotary_cache: bfloat16 [8, 1024, 64], P('sp', None, 'tp')
- first_read: bfloat16 [8, 16, 128], P('sp', 'tp')
The draws below stay inside these ranges and needn't reach their ends.
All inputs are finite; a program needn't handle non-finite values.
Results may differ from the reference program's by a relative error of at most 0.02.
Values may be sent and summed in bfloat16 or wider, within the bound.
A program may use at most 64 MiB of HBM per device.

```python
import jax
import jax.numpy as jnp
from jax import lax

BREADTH = 2048
SQUEEZED_SPAN = 512
QK_ROPE = 64
PLAIN_MATCH_SPAN = 128
PAYLOAD_SPAN = 128
READERS = 16
BATCH_ITEMS = 8
SLOTS = 1024


def block_scale(stream_key, dims, shards, least, largest):
    def one(axis_at, blocks):
        heights = jax.random.uniform(jax.random.fold_in(jax.random.fold_in(stream_key, 6), axis_at), (blocks,), jnp.float32, least / len(shards), largest / len(shards))
        return jnp.repeat(jnp.exp(heights), dims[axis_at] // blocks).reshape((-1,) + (1,) * (len(dims) - axis_at - 1))

    factor_of = one(*shards[0])
    for cut in shards[1:]:
        factor_of = factor_of * one(*cut)
    return factor_of


def normal_values(stream_key, extent, deviation, reach, shards=(), held_as=jnp.bfloat16):
    level = block_scale(stream_key, extent, shards, -0.22, 0.18) if shards else 1.0
    entries = jax.random.normal(stream_key, extent, jnp.float32) * deviation * level
    return jnp.minimum(jnp.maximum(entries, -reach), reach).astype(held_as)


def setup_inputs(seed: int = 0) -> dict:
    keys = jax.random.split(jax.random.key(seed), 10)
    layer_input = normal_values(keys[0], (BATCH_ITEMS, SLOTS, BREADTH), 1.0, 6.0, ((1, 32),))
    input_gain = jnp.clip(1.0 + 0.1 * jax.random.normal(keys[1], (BREADTH,), jnp.float32), 0.5, 1.5)
    narrowing_matrix = normal_values(keys[2], (BREADTH, SQUEEZED_SPAN), BREADTH ** -0.5, 0.125)
    rotary_down = normal_values(keys[3], (BREADTH, QK_ROPE), BREADTH ** -0.5, 0.125)
    summary_scaling = jnp.clip(1.0 + 0.1 * jax.random.normal(keys[4], (SQUEEZED_SPAN,), jnp.float32), 0.5, 1.5)
    lookup_widening = normal_values(keys[5], (SQUEEZED_SPAN, READERS, PLAIN_MATCH_SPAN), SQUEEZED_SPAN ** -0.5, 0.25, ((0, 4),))
    payload_widening = normal_values(keys[6], (SQUEEZED_SPAN, READERS, PAYLOAD_SPAN), SQUEEZED_SPAN ** -0.5, 0.25, ((0, 4),))
    query_nope = normal_values(keys[7], (BATCH_ITEMS, READERS, PLAIN_MATCH_SPAN), 1.0, 6.0, ((0, 8), (1, 4)))
    query_rotary = normal_values(keys[8], (BATCH_ITEMS, READERS, QK_ROPE), 1.0, 6.0, ((0, 8), (1, 4)))
    return {"layer_input": layer_input, "input_gain": input_gain, "narrowing_matrix": narrowing_matrix, "rotary_down": rotary_down, "summary_scaling": summary_scaling, "lookup_widening": lookup_widening, "payload_widening": payload_widening, "query_nope": query_nope, "query_rotary": query_rotary}


norm_eps = 1e-06
rotary_base = 10000.0

def rescaled_lines(vector):
    return vector * lax.rsqrt(lax.optimization_barrier(jnp.mean(vector * vector, axis=-1, keepdims=True)) + norm_eps)

def rotate(vector, position):
    half_width = vector.shape[-1] // 2
    frequency = 1.0 / rotary_base ** (jnp.arange(half_width, dtype=jnp.float32) * 2.0 / vector.shape[-1])
    angles = position * frequency
    first_half = vector[..., :half_width]
    second_half = vector[..., half_width:]
    return jnp.concatenate([first_half * jnp.cos(angles) - second_half * jnp.sin(angles), second_half * jnp.cos(angles) + first_half * jnp.sin(angles)], axis=-1)

def reference(layer_input, input_gain, narrowing_matrix, rotary_down, summary_scaling, lookup_widening, payload_widening, query_nope, query_rotary):
    normed = (rescaled_lines(layer_input.astype(jnp.float32)) * input_gain).astype(jnp.bfloat16)
    flat_rows = normed.reshape(BATCH_ITEMS * SLOTS, BREADTH)
    hidden_summary = jnp.dot(flat_rows, narrowing_matrix, preferred_element_type=jnp.float32).astype(jnp.bfloat16)
    rotary = jnp.dot(flat_rows, rotary_down, preferred_element_type=jnp.float32).astype(jnp.bfloat16)
    stored_summaries = (rescaled_lines(hidden_summary.astype(jnp.float32)) * summary_scaling).astype(jnp.bfloat16).reshape(BATCH_ITEMS, SLOTS, SQUEEZED_SPAN)
    positions = jnp.arange(SLOTS, dtype=jnp.float32)[None, :, None]
    rotary_cache = rotate(rotary.astype(jnp.float32).reshape(BATCH_ITEMS, SLOTS, QK_ROPE), positions).astype(jnp.bfloat16)
    absorbed = jnp.einsum('shd,chd->shc', query_nope.astype(jnp.float32), lookup_widening.astype(jnp.float32)).astype(jnp.bfloat16)
    query_turned = rotate(query_rotary.astype(jnp.float32), jnp.float32(SLOTS)).astype(jnp.bfloat16)
    score_scale = (PLAIN_MATCH_SPAN + QK_ROPE) ** (-0.5)
    scores = (jnp.einsum('shc,spc->shp', absorbed.astype(jnp.float32), stored_summaries.astype(jnp.float32)) + jnp.einsum('shr,spr->shp', query_turned.astype(jnp.float32), rotary_cache.astype(jnp.float32))) * score_scale
    attention = jax.nn.softmax(scores, axis=-1).astype(jnp.bfloat16)
    context = jnp.einsum('shp,spc->shc', attention.astype(jnp.float32), stored_summaries.astype(jnp.float32)).astype(jnp.bfloat16)
    values = jnp.einsum('shc,chv->shv', context.astype(jnp.float32), payload_widening.astype(jnp.float32))
    first_read = rescaled_lines(values).astype(jnp.bfloat16)
    return (stored_summaries, rotary_cache, first_read)
```

```python
import functools

import jax
import jax.numpy as jnp
from jax import lax
from jax.experimental import pallas as pl
from jax.experimental.pallas import tpu as pltpu
from jax.sharding import PartitionSpec as P

QK_ROPE = 64
PLAIN_MATCH_SPAN = 128

norm_eps = 1e-06
rotary_base = 10000.0
LANES = 128
ROW_CHUNKS = 2
K_CHUNKS = 4
MESH = pl.DeviceIdType.MESH
f32 = jnp.float32
bf16 = jnp.bfloat16


def rescaled_lines(vector):
    return vector * lax.rsqrt(jnp.mean(vector * vector, axis=-1, keepdims=True) + norm_eps)


def iota(shape, axis):
    return lax.broadcasted_iota(jnp.int32, shape, axis)


def one_hot(cond):
    return jnp.where(cond, 1.0, 0.0).astype(bf16)


def dot(a, b):
    return jnp.dot(a, b, preferred_element_type=f32)


def dot_t(a, b):
    return lax.dot_general(a, b, (((1,), (1,)), ((), ())), preferred_element_type=f32)


def kernel(
    dims,
    x_hbm,
    w_hbm,
    wr_hbm,
    lw_hbm,
    pw_hbm,
    gain_ref,
    sgain_ref,
    table_ref,
    q_ref,
    qr_ref,
    cache_out,
    rotary_out,
    read_out,
    x_ref,
    w_ref,
    wr_ref,
    lw_ref,
    pw_ref,
    xn_ref,
    stage,
    rstage,
    lat_recv,
    rot_recv,
    q_recv,
    q_all,
    s_recv,
    v_send,
    v_recv,
    spread,
    unpack,
    rot_full,
    load_sem,
    out_sem,
    lat_sem,
    rot_sem,
    q_send_sem,
    q_recv_sem,
    s_send_sem,
    s_recv_sem,
    v_send_sem,
    v_recv_sem,
):
    sp_count, tp_count = dims
    n = sp_count * tp_count
    seq_count, pos_local, features = x_ref.shape
    latent = w_ref.shape[1]
    rope = wr_ref.shape[0]
    width = latent // tp_count
    rot_each = rope // tp_count
    packs = LANES // rot_each
    prow = pos_local // packs
    head_each, plain = q_ref.shape
    heads = head_each * tp_count
    total = n * pos_local
    my_sp = lax.axis_index("sp")
    my_tp = lax.axis_index("tp")
    me = my_sp * tp_count + my_tp

    loads = {}

    def load(key, index, src, dst):
        copy = pltpu.make_async_copy(src, dst, load_sem.at[index])
        copy.start()
        loads[key] = copy

    kdepth = features // K_CHUNKS
    for j in range(seq_count):
        load(("x", j), j, x_hbm.at[lax.rem(my_sp + 1 + j, sp_count)], x_ref.at[j])
    for k in range(K_CHUNKS):
        rows = pl.ds(k * kdepth, kdepth)
        load(("w", k), seq_count + k, w_hbm.at[rows], w_ref.at[rows])
    base = seq_count + K_CHUNKS
    load("wr", base, wr_hbm, wr_ref)
    load("lw", base + 1, lw_hbm, lw_ref)
    load("pw", base + 2, pw_hbm, pw_ref)

    barrier = pltpu.get_barrier_semaphore()

    def greet(i, carry):
        other = lax.rem(me + 1 + i, n)
        pl.semaphore_signal(
            barrier,
            inc=1,
            device_id=(lax.div(other, tp_count), lax.rem(other, tp_count)),
            device_id_type=MESH,
        )
        return carry

    lax.fori_loop(0, n - 1, greet, 0)

    q_recv[my_tp] = jnp.zeros(q_recv.shape[1:], f32)
    q_recv[my_tp, :, :plain] = q_ref[...].astype(f32)
    q_recv[my_tp, :, plain : plain + rope] = qr_ref[...].astype(f32)

    cos = table_ref[0, :pos_local, :]
    sin = table_ref[1, :pos_local, :]
    half = rope // 2
    row_r, col_r = iota((rope, rope), 0), iota((rope, rope), 1)
    swap = (
        jnp.where((row_r == col_r + half), -1.0, 0.0)
        + jnp.where((row_r + half == col_r), 1.0, 0.0)
    ).astype(bf16)
    wide = (rope, tp_count * LANES)
    tile = one_hot(
        iota(wide, 0)
        == iota(wide, 1) // LANES * rot_each + iota(wide, 1) % rot_each
    )

    pairs = []

    def remote(src, dst, send, recv, sp, tp):
        copy = pltpu.make_async_remote_copy(
            src_ref=src,
            dst_ref=dst,
            send_sem=send,
            recv_sem=recv,
            device_id=(sp, tp),
            device_id_type=MESH,
        )
        copy.start()
        return copy

    chunk_seq = seq_count // ROW_CHUNKS
    chunk = chunk_seq * pos_local
    pick_shape = (chunk_seq * prow, chunk)
    pick_row, pick_col = iota(pick_shape, 0), iota(pick_shape, 1)
    pick = one_hot(
        (pick_row // prow == pick_col // pos_local) & (pick_row % prow == pick_col % prow)
    )
    mask_shape = (chunk, tp_count * LANES)
    keep = (iota(mask_shape, 1) % LANES) // rot_each == (
        iota(mask_shape, 0) % pos_local
    ) // prow

    for c in range(ROW_CHUNKS):
        for j in range(chunk_seq):
            at = c * chunk_seq + j
            loads[("x", at)].wait()
            rows = rescaled_lines(x_ref[at].astype(f32)) * gain_ref[...]
            xn_ref[pl.ds(j * pos_local, pos_local), :] = rows.astype(bf16)
        acc = None
        for k in range(K_CHUNKS):
            if c == 0:
                loads[("w", k)].wait()
            part = dot(
                xn_ref[:, k * kdepth : (k + 1) * kdepth],
                w_ref[k * kdepth : (k + 1) * kdepth, :],
            )
            acc = part if acc is None else acc + part
        if c == 0:
            loads["wr"].wait()
        rot = dot_t(xn_ref[...], wr_ref[...]).astype(bf16)
        hidden = rescaled_lines(acc.astype(bf16).astype(f32)) * sgain_ref[...]
        swapped = dot(rot, swap)
        turned = (
            rot.astype(f32).reshape(chunk_seq, pos_local, rope) * cos[None]
            + swapped.reshape(chunk_seq, pos_local, rope) * sin[None]
        ).reshape(chunk, rope)
        copies = dot(turned.astype(bf16), tile)
        packed = dot(pick, jnp.where(keep, copies, 0.0).astype(bf16))
        for j in range(chunk_seq):
            for t in range(tp_count):
                at = (c * chunk_seq + j) * tp_count + t
                stage[at] = hidden[
                    j * pos_local : (j + 1) * pos_local, t * width : (t + 1) * width
                ].astype(bf16)
                rstage[at] = packed[
                    j * prow : (j + 1) * prow, t * LANES : (t + 1) * LANES
                ].astype(bf16)
        if c == 0:
            pl.semaphore_wait(barrier, n - 1)
            for k in range(tp_count - 1):
                peer = lax.rem(my_tp + 1 + k, tp_count)
                pairs.append(
                    remote(
                        q_recv.at[my_tp],
                        q_recv.at[my_tp],
                        q_send_sem.at[k],
                        q_recv_sem.at[k],
                        my_sp,
                        peer,
                    )
                )
        for j in range(chunk_seq):
            order = c * chunk_seq + j
            to_sp = lax.rem(my_sp + 1 + order, sp_count)
            for k in range(tp_count):
                to_tp = lax.rem(my_tp + 1 + k, tp_count)
                at = order * tp_count + to_tp
                if order == seq_count - 1 and k == tp_count - 1:
                    lat_recv[me] = stage[at]
                    rot_recv[me] = rstage[at]
                else:
                    remote(
                        rstage.at[at], rot_recv.at[me], rot_sem.at[0], rot_sem.at[1], to_sp, to_tp
                    )
                    remote(
                        stage.at[at], lat_recv.at[me], lat_sem.at[0], lat_sem.at[1], to_sp, to_tp
                    )

    spread_shape = spread.shape
    spread[...] = one_hot(iota(spread_shape, 0) // heads == iota(spread_shape, 1))
    own_shape = (heads, width * heads)
    own_head = iota(own_shape, 0) == iota(own_shape, 1) % heads
    un_shape = unpack.shape
    un_row, un_col = iota(un_shape, 0), iota(un_shape, 1)
    unpack[...] = one_hot(
        (un_row // pos_local == un_col // prow) & (un_row % prow == un_col % prow)
    )
    rkeep_shape = (total, LANES)
    rkeep = iota(rkeep_shape, 1) // rot_each == (iota(rkeep_shape, 0) % pos_local) // prow
    narrow = (LANES, rot_each)
    fold = one_hot(iota(narrow, 0) % rot_each == iota(narrow, 1))

    for copy in pairs:
        copy.wait()
    for t in range(tp_count):
        q_all[t * head_each : (t + 1) * head_each, :] = q_recv[t]
    queries = q_all[:, :plain].astype(bf16)
    q_rot = q_all[:, plain : plain + rope]
    qcos = table_ref[0, pos_local : pos_local + 1, :]
    qsin = table_ref[1, pos_local : pos_local + 1, :]
    q_turned = (q_rot * qcos + dot(q_rot.astype(bf16), swap) * qsin).astype(bf16)
    share = (rope, rot_each)
    mine = one_hot(iota(share, 0) == iota(share, 1) + my_tp * rot_each)
    q_mine = dot(q_turned, mine).astype(bf16)
    loads["lw"].wait()
    lookup = lw_ref[...].reshape(width * heads, plain)
    every = dot_t(queries, lookup)
    absorbed = dot(jnp.where(own_head, every, 0.0).astype(bf16), spread[...]).astype(bf16)

    pltpu.make_async_copy(
        rot_recv.at[pl.ds(0, n - 1)], rot_recv.at[pl.ds(0, n - 1)], rot_sem.at[1]
    ).wait()
    rot_rows = rot_recv[...].astype(f32).reshape(n * prow, LANES).astype(bf16)
    rot_wide = jnp.where(rkeep, dot(unpack[...], rot_rows), 0.0).astype(bf16)
    rot_cache = dot(rot_wide, fold).astype(bf16)
    rot_full[...] = rot_cache
    rot_store = pltpu.make_async_copy(rot_full, rotary_out, out_sem.at[1])
    rot_store.start()
    rot_part = dot_t(q_mine, rot_cache)

    pltpu.make_async_copy(
        lat_recv.at[pl.ds(0, n - 1)], lat_recv.at[pl.ds(0, n - 1)], lat_sem.at[1]
    ).wait()
    cache_store = pltpu.make_async_copy(lat_recv, cache_out, out_sem.at[0])
    cache_store.start()
    cache = lat_recv[...].reshape(total, width)
    score_scale = (PLAIN_MATCH_SPAN + QK_ROPE) ** (-0.5)
    s_recv[my_tp] = ((dot_t(absorbed, cache) + rot_part) * score_scale).astype(bf16)
    pairs = []
    for k in range(tp_count - 1):
        peer = lax.rem(my_tp + 1 + k, tp_count)
        pairs.append(
            remote(
                s_recv.at[my_tp],
                s_recv.at[my_tp],
                s_send_sem.at[k],
                s_recv_sem.at[k],
                my_sp,
                peer,
            )
        )
    loads["pw"].wait()
    for copy in pairs:
        copy.wait()
    scores = s_recv[0].astype(f32)
    for t in range(1, tp_count):
        scores = scores + s_recv[t].astype(f32)
    top = jnp.max(scores, axis=-1, keepdims=True)
    weights = jnp.exp(scores - top)
    attention = (weights / jnp.sum(weights, axis=-1, keepdims=True)).astype(bf16)
    context = dot(attention, cache).astype(bf16)
    laid = jnp.where(own_head, dot_t(context, spread[...]), 0.0).astype(bf16)
    payload = pw_ref[...].reshape(width * heads, pw_ref.shape[2])
    values = dot(laid, payload)
    for t in range(tp_count):
        v_send[t] = values[t * head_each : (t + 1) * head_each, :]
    v_recv[my_tp] = v_send[my_tp]
    pairs = []
    for k in range(tp_count - 1):
        peer = lax.rem(my_tp + 1 + k, tp_count)
        pairs.append(
            remote(
                v_send.at[peer],
                v_recv.at[my_tp],
                v_send_sem.at[k],
                v_recv_sem.at[k],
                my_sp,
                peer,
            )
        )
    pltpu.make_async_copy(
        rstage.at[pl.ds(0, n - 1)], rstage.at[pl.ds(0, n - 1)], rot_sem.at[0]
    ).wait()
    pltpu.make_async_copy(
        stage.at[pl.ds(0, n - 1)], stage.at[pl.ds(0, n - 1)], lat_sem.at[0]
    ).wait()
    cache_store.wait()
    rot_store.wait()
    for copy in pairs:
        copy.wait()
    summed = v_recv[0]
    for t in range(1, tp_count):
        summed = summed + v_recv[t]
    read_out[...] = rescaled_lines(summed).astype(bf16)


def shards(
    layer_input,
    input_gain,
    narrowing_matrix,
    rotary_down,
    summary_scaling,
    lookup_widening,
    payload_widening,
    query_nope,
    query_rotary,
):
    seq_count, pos_local, features = layer_input.shape
    sp_count = lax.axis_size("sp")
    tp_count = lax.axis_size("tp")
    n = sp_count * tp_count
    assert seq_count == sp_count
    latent = narrowing_matrix.shape[1]
    rope = rotary_down.shape[1]
    width, heads, plain = lookup_widening.shape
    payload = payload_widening.shape[2]
    head_each = query_nope.shape[1]
    rot_each = rope // tp_count
    prow = pos_local * rot_each // LANES
    total = n * pos_local
    block_index = lax.axis_index(("sp", "tp"))
    half = rope // 2
    frequency = 1.0 / rotary_base ** (jnp.arange(half, dtype=f32) * 2.0 / rope)
    frequency = jnp.concatenate([frequency, frequency])
    spots = jnp.arange(pos_local + 8, dtype=jnp.int32)
    spots = jnp.where(spots < pos_local, block_index * pos_local + spots, total)
    angles = spots.astype(f32)[:, None] * frequency[None, :]
    table = jnp.stack([jnp.cos(angles), jnp.sin(angles)])
    any_spec = pl.BlockSpec(memory_space=pl.ANY)
    vmem_spec = pl.BlockSpec(memory_space=pltpu.VMEM)
    dma = pltpu.SemaphoreType.DMA
    cache, rotary, read = pl.pallas_call(
        functools.partial(kernel, (sp_count, tp_count)),
        out_shape=(
            jax.ShapeDtypeStruct((n, pos_local, width), bf16),
            jax.ShapeDtypeStruct((total, rot_each), bf16),
            jax.ShapeDtypeStruct((head_each, payload), bf16),
        ),
        in_specs=[any_spec] * 5 + [vmem_spec] * 5,
        out_specs=(any_spec, any_spec, vmem_spec),
        scratch_shapes=[
            pltpu.VMEM((seq_count, pos_local, features), bf16),
            pltpu.VMEM((features, latent), bf16),
            pltpu.VMEM((rope, features), bf16),
            pltpu.VMEM((width, heads, plain), bf16),
            pltpu.VMEM((width, heads, payload), bf16),
            pltpu.VMEM((seq_count * pos_local // ROW_CHUNKS, features), bf16),
            pltpu.VMEM((n, pos_local, width), bf16),
            pltpu.VMEM((n, prow, LANES), bf16),
            pltpu.VMEM((n, pos_local, width), bf16),
            pltpu.VMEM((n, prow, LANES), bf16),
            pltpu.VMEM((tp_count, head_each, 2 * LANES), f32),
            pltpu.VMEM((heads, 2 * LANES), f32),
            pltpu.VMEM((tp_count, heads, total), bf16),
            pltpu.VMEM((tp_count, head_each, payload), f32),
            pltpu.VMEM((tp_count, head_each, payload), f32),
            pltpu.VMEM((width * heads, width), bf16),
            pltpu.VMEM((total, n * prow), bf16),
            pltpu.VMEM((total, rot_each), bf16),
            dma((seq_count + K_CHUNKS + 3,)),
            dma((2,)),
            dma((2,)),
            dma((2,)),
            dma((tp_count - 1,)),
            dma((tp_count - 1,)),
            dma((tp_count - 1,)),
            dma((tp_count - 1,)),
            dma((tp_count - 1,)),
            dma((tp_count - 1,)),
        ],
        compiler_params=pltpu.CompilerParams(
            collective_id=0, has_side_effects=True, vmem_limit_bytes=63 * 1024 * 1024
        ),
    )(
        layer_input,
        narrowing_matrix,
        rotary_down.T,
        lookup_widening,
        payload_widening,
        input_gain.reshape(1, -1),
        summary_scaling.reshape(1, -1),
        table,
        query_nope[0],
        query_rotary[0],
    )
    return (
        cache.reshape(1, total, width),
        rotary.reshape(1, total, rot_each),
        read.reshape(1, head_each, payload),
    )


def solution(mesh):
    return jax.shard_map(
        shards,
        mesh=mesh,
        in_specs=(
            P(None, ("sp", "tp"), None),
            P(),
            P(),
            P(),
            P(),
            P("tp", None, None),
            P("tp", None, None),
            P("sp", "tp", None),
            P("sp", "tp", None),
        ),
        out_specs=(P("sp", None, "tp"), P("sp", None, "tp"), P("sp", "tp", None)),
        check_vma=False,
    )
```

```python
import functools

import jax
import jax.numpy as jnp
import numpy as np
from jax import lax
from jax.experimental import pallas as pl
from jax.experimental.pallas import tpu as pltpu
from jax.sharding import PartitionSpec as P

QK_ROPE = 64
PLAIN_MATCH_SPAN = 128

norm_eps = 1e-06
rotary_base = 10000.0
LANES = 128
VMEM_BYTES = 67043328
ROW_CHUNKS = 2
K_CHUNKS = 4
MESH = pl.DeviceIdType.MESH
f32 = jnp.float32
bf16 = jnp.bfloat16


def rescaled_lines(vector):
    return vector * lax.rsqrt(jnp.mean(vector * vector, axis=-1, keepdims=True) + norm_eps)


def iota(shape, axis):
    return lax.broadcasted_iota(jnp.int32, shape, axis)


def one_hot(cond):
    return jnp.where(cond, 1.0, 0.0).astype(bf16)


def dot(a, b):
    return jnp.dot(a, b, preferred_element_type=f32)


def dot_t(a, b):
    return lax.dot_general(a, b, (((1,), (1,)), ((), ())), preferred_element_type=f32)


def kernel(
    dims,
    x_hbm,
    w_hbm,
    wr_hbm,
    lw_hbm,
    pw_hbm,
    table_hbm,
    gain_ref,
    sgain_ref,
    q_ref,
    qr_ref,
    cache_out,
    rotary_out,
    read_out,
    x_ref,
    w_ref,
    wr_ref,
    lw_ref,
    pw_ref,
    xn_ref,
    stage,
    rstage,
    lat_recv,
    rot_recv,
    q_recv,
    q_all,
    s_recv,
    v_send,
    v_recv,
    spread,
    unpack,
    table_ref,
    load_sem,
    lat_sem,
    rot_sem,
    q_send_sem,
    q_recv_sem,
    s_send_sem,
    s_recv_sem,
    v_send_sem,
    v_recv_sem,
):
    sp_count, tp_count = dims
    n = sp_count * tp_count
    seq_count, pos_local, features = x_ref.shape
    latent = w_ref.shape[1]
    rope = wr_ref.shape[0]
    width = latent // tp_count
    rot_each = rope // tp_count
    packs = LANES // rot_each
    prow = pos_local // packs
    head_each, plain = q_ref.shape
    heads = head_each * tp_count
    total = n * pos_local
    my_sp = lax.axis_index("sp")
    my_tp = lax.axis_index("tp")
    me = my_sp * tp_count + my_tp

    loads = {}

    def load(key, index, src, dst):
        copy = pltpu.make_async_copy(src, dst, load_sem.at[index])
        copy.start()
        loads[key] = copy

    kdepth = features // K_CHUNKS
    half_sp = sp_count // 2
    my_half = lax.div(my_sp, half_sp)
    in_half = lax.rem(my_sp, half_sp)

    def target(order):
        if order < half_sp:
            return (1 - my_half) * half_sp + lax.rem(in_half + order, half_sp)
        return my_half * half_sp + lax.rem(in_half + 1 + order - half_sp, half_sp)

    for j in range(seq_count):
        load(("x", j), j, x_hbm.at[target(j)], x_ref.at[j])
    for k in range(K_CHUNKS):
        rows = pl.ds(k * kdepth, kdepth)
        load(("w", k), seq_count + k, w_hbm.at[rows], w_ref.at[rows])
    base = seq_count + K_CHUNKS
    load("wr", base, wr_hbm, wr_ref)
    load("lw", base + 1, lw_hbm, lw_ref)
    load("pw", base + 2, pw_hbm, pw_ref)
    load(
        "table",
        base + 3,
        table_hbm.at[:, pl.ds(me * pos_local, pos_local)],
        table_ref.at[:, pl.ds(0, pos_local)],
    )
    load(
        "last",
        base + 4,
        table_hbm.at[:, pl.ds(total, 8)],
        table_ref.at[:, pl.ds(pos_local, 8)],
    )

    barrier = pltpu.get_barrier_semaphore()

    def greet(i, carry):
        other = lax.rem(me + 1 + i, n)
        pl.semaphore_signal(
            barrier,
            inc=1,
            device_id=(lax.div(other, tp_count), lax.rem(other, tp_count)),
            device_id_type=MESH,
        )
        return carry

    lax.fori_loop(0, n - 1, greet, 0)

    q_recv[my_tp] = jnp.zeros(q_recv.shape[1:], f32)
    q_recv[my_tp, :, :plain] = q_ref[...].astype(f32)
    q_recv[my_tp, :, plain : plain + rope] = qr_ref[...].astype(f32)

    half = rope // 2
    row_r, col_r = iota((rope, rope), 0), iota((rope, rope), 1)
    swap = (
        jnp.where((row_r == col_r + half), -1.0, 0.0)
        + jnp.where((row_r + half == col_r), 1.0, 0.0)
    ).astype(bf16)
    wide = (rope, tp_count * LANES)
    tile = one_hot(
        iota(wide, 0)
        == iota(wide, 1) // LANES * rot_each + iota(wide, 1) % rot_each
    )

    pairs = []

    def remote(src, dst, send, recv, sp, tp):
        copy = pltpu.make_async_remote_copy(
            src_ref=src,
            dst_ref=dst,
            send_sem=send,
            recv_sem=recv,
            device_id=(sp, tp),
            device_id_type=MESH,
        )
        copy.start()
        return copy

    chunk_seq = seq_count // ROW_CHUNKS
    chunk = chunk_seq * pos_local
    pick_shape = (chunk_seq * prow, chunk)
    pick_row, pick_col = iota(pick_shape, 0), iota(pick_shape, 1)
    pick = one_hot(
        (pick_row // prow == pick_col // pos_local) & (pick_row % prow == pick_col % prow)
    )
    mask_shape = (chunk, tp_count * LANES)
    keep = (iota(mask_shape, 1) % LANES) // rot_each == (
        iota(mask_shape, 0) % pos_local
    ) // prow

    for c in range(ROW_CHUNKS):
        for j in range(chunk_seq):
            at = c * chunk_seq + j
            loads[("x", at)].wait()
            rows = rescaled_lines(x_ref[at].astype(f32)) * gain_ref[...]
            xn_ref[pl.ds(j * pos_local, pos_local), :] = rows.astype(bf16)
        acc = None
        for k in range(K_CHUNKS):
            if c == 0:
                loads[("w", k)].wait()
            part = dot(
                xn_ref[:, k * kdepth : (k + 1) * kdepth],
                w_ref[k * kdepth : (k + 1) * kdepth, :],
            )
            acc = part if acc is None else acc + part
        if c == 0:
            loads["wr"].wait()
            loads["table"].wait()
            loads["last"].wait()
        cos = table_ref[0, :pos_local, :]
        sin = table_ref[1, :pos_local, :]
        rot = dot_t(xn_ref[...], wr_ref[...]).astype(bf16)
        hidden = rescaled_lines(acc.astype(bf16).astype(f32)) * sgain_ref[...]
        swapped = dot(rot, swap)
        turned = (
            rot.astype(f32).reshape(chunk_seq, pos_local, rope) * cos[None]
            + swapped.reshape(chunk_seq, pos_local, rope) * sin[None]
        ).reshape(chunk, rope)
        copies = dot(turned.astype(bf16), tile)
        packed = dot(pick, jnp.where(keep, copies, 0.0).astype(bf16))
        for j in range(chunk_seq):
            for t in range(tp_count):
                at = (c * chunk_seq + j) * tp_count + t
                stage[at] = hidden[
                    j * pos_local : (j + 1) * pos_local, t * width : (t + 1) * width
                ].astype(bf16)
                rstage[at] = packed[
                    j * prow : (j + 1) * prow, t * LANES : (t + 1) * LANES
                ].astype(bf16)
        if c == 0:
            pl.semaphore_wait(barrier, n - 1)
            for k in range(tp_count - 1):
                peer = lax.rem(my_tp + 1 + k, tp_count)
                pairs.append(
                    remote(
                        q_recv.at[my_tp],
                        q_recv.at[my_tp],
                        q_send_sem.at[k],
                        q_recv_sem.at[k],
                        my_sp,
                        peer,
                    )
                )
        for j in range(chunk_seq):
            order = c * chunk_seq + j
            to_sp = target(order)
            for k in range(tp_count):
                to_tp = lax.rem(my_tp + 1 + k, tp_count)
                at = order * tp_count + to_tp
                if order == seq_count - 1 and k == tp_count - 1:
                    lat_recv[me] = stage[at]
                    rot_recv[me] = rstage[at]
                else:
                    remote(
                        rstage.at[at], rot_recv.at[me], rot_sem.at[0], rot_sem.at[1], to_sp, to_tp
                    )
                    remote(
                        stage.at[at], lat_recv.at[me], lat_sem.at[0], lat_sem.at[1], to_sp, to_tp
                    )

    spread_shape = spread.shape
    spread[...] = one_hot(iota(spread_shape, 0) // heads == iota(spread_shape, 1))
    own_shape = (heads, width * heads)
    own_head = iota(own_shape, 0) == iota(own_shape, 1) % heads
    un_shape = unpack.shape
    un_row, un_col = iota(un_shape, 0), iota(un_shape, 1)
    unpack[...] = one_hot(
        (un_row // pos_local == un_col // prow) & (un_row % prow == un_col % prow)
    )
    rkeep_shape = (total, LANES)
    rkeep = iota(rkeep_shape, 1) // rot_each == (iota(rkeep_shape, 0) % pos_local) // prow
    narrow = (rot_each, LANES)
    fold = one_hot(iota(narrow, 1) % rot_each == iota(narrow, 0))

    for copy in pairs:
        copy.wait()
    for t in range(tp_count):
        q_all[t * head_each : (t + 1) * head_each, :] = q_recv[t]
    queries = q_all[:, :plain].astype(bf16)
    q_rot = q_all[:, plain : plain + rope]
    qcos = table_ref[0, pos_local : pos_local + 1, :]
    qsin = table_ref[1, pos_local : pos_local + 1, :]
    q_turned = (q_rot * qcos + dot(q_rot.astype(bf16), swap) * qsin).astype(bf16)
    share = (rope, rot_each)
    mine = one_hot(iota(share, 0) == iota(share, 1) + my_tp * rot_each)
    q_mine = dot(q_turned, mine).astype(bf16)
    loads["lw"].wait()
    lookup = lw_ref[...].reshape(width * heads, plain)
    every = dot_t(queries, lookup)
    absorbed = dot(jnp.where(own_head, every, 0.0).astype(bf16), spread[...]).astype(bf16)

    pltpu.make_async_copy(
        rot_recv.at[pl.ds(0, n - 1)], rot_recv.at[pl.ds(0, n - 1)], rot_sem.at[1]
    ).wait()
    rot_rows = rot_recv[...].astype(f32).reshape(n * prow, LANES).astype(bf16)
    rot_wide = jnp.where(rkeep, dot(unpack[...], rot_rows), 0.0).astype(bf16)
    rot_cache = dot_t(fold, rot_wide).astype(bf16)
    rotary_out[...] = rot_cache
    rot_part = dot(q_mine, rot_cache)

    pltpu.make_async_copy(
        lat_recv.at[pl.ds(0, n - 1)], lat_recv.at[pl.ds(0, n - 1)], lat_sem.at[1]
    ).wait()
    cache = lat_recv[...].reshape(total, width)
    score_scale = (PLAIN_MATCH_SPAN + QK_ROPE) ** (-0.5)
    s_recv[my_tp] = ((dot_t(absorbed, cache) + rot_part) * score_scale).astype(bf16)
    pairs = []
    for k in range(tp_count - 1):
        peer = lax.rem(my_tp + 1 + k, tp_count)
        pairs.append(
            remote(
                s_recv.at[my_tp],
                s_recv.at[my_tp],
                s_send_sem.at[k],
                s_recv_sem.at[k],
                my_sp,
                peer,
            )
        )
    loads["pw"].wait()
    for copy in pairs:
        copy.wait()
    scores = s_recv[0].astype(f32)
    for t in range(1, tp_count):
        scores = scores + s_recv[t].astype(f32)
    top = jnp.max(scores, axis=-1, keepdims=True)
    weights = jnp.exp(scores - top)
    attention = (weights / jnp.sum(weights, axis=-1, keepdims=True)).astype(bf16)
    context = dot(attention, cache).astype(bf16)
    laid = jnp.where(own_head, dot_t(context, spread[...]), 0.0).astype(bf16)
    payload = pw_ref[...].reshape(width * heads, pw_ref.shape[2])
    values = dot(laid, payload)
    for t in range(tp_count):
        v_send[t] = values[t * head_each : (t + 1) * head_each, :]
    v_recv[my_tp] = v_send[my_tp]
    pairs = []
    for k in range(tp_count - 1):
        peer = lax.rem(my_tp + 1 + k, tp_count)
        pairs.append(
            remote(
                v_send.at[peer],
                v_recv.at[my_tp],
                v_send_sem.at[k],
                v_recv_sem.at[k],
                my_sp,
                peer,
            )
        )
    pltpu.make_async_copy(
        rstage.at[pl.ds(0, n - 1)], rstage.at[pl.ds(0, n - 1)], rot_sem.at[0]
    ).wait()
    pltpu.make_async_copy(
        stage.at[pl.ds(0, n - 1)], stage.at[pl.ds(0, n - 1)], lat_sem.at[0]
    ).wait()
    cache_out[...] = lat_recv[...]
    for copy in pairs:
        copy.wait()
    summed = v_recv[0]
    for t in range(1, tp_count):
        summed = summed + v_recv[t]
    read_out[...] = rescaled_lines(summed).astype(bf16)


def rotary_table(total, rope):
    half = rope // 2
    frequency = 1.0 / rotary_base ** (np.arange(half) * 2.0 / rope)
    frequency = np.concatenate([frequency, frequency]).astype(np.float32)
    spots = np.minimum(np.arange(total + 8), total).astype(np.float32)
    angles = (spots[:, None] * frequency[None, :]).astype(np.float64)
    return np.stack([np.cos(angles), np.sin(angles)]).astype(np.float32)


def write_out(cache_ref, rotary_ref, read_ref, cache_hbm, rotary_hbm, read_hbm, sems):
    copies = [
        pltpu.make_async_copy(src, dst, sems.at[i])
        for i, (src, dst) in enumerate(
            ((cache_ref, cache_hbm), (rotary_ref, rotary_hbm), (read_ref, read_hbm))
        )
    ]
    for copy in copies:
        copy.start()
    for copy in copies:
        copy.wait()


def shards(
    layer_input,
    input_gain,
    narrowing_matrix,
    rotary_down,
    summary_scaling,
    lookup_widening,
    payload_widening,
    query_nope,
    query_rotary,
):
    seq_count, pos_local, features = layer_input.shape
    sp_count = lax.axis_size("sp")
    tp_count = lax.axis_size("tp")
    n = sp_count * tp_count
    assert seq_count == sp_count
    latent = narrowing_matrix.shape[1]
    rope = rotary_down.shape[1]
    width, heads, plain = lookup_widening.shape
    payload = payload_widening.shape[2]
    head_each = query_nope.shape[1]
    rot_each = rope // tp_count
    prow = pos_local * rot_each // LANES
    total = n * pos_local
    table = jnp.asarray(rotary_table(total, rope))
    held = 2 * total * (max(width, LANES) + max(rot_each, 16)) + 52 * 1024
    hbm_spec = pl.BlockSpec(memory_space=pltpu.HBM)
    vmem_spec = pl.BlockSpec(memory_space=pltpu.VMEM)
    dma = pltpu.SemaphoreType.DMA
    cache, rotary, read = pl.pallas_call(
        functools.partial(kernel, (sp_count, tp_count)),
        out_shape=(
            pltpu.VMEM((n, pos_local, width), bf16),
            pltpu.VMEM((rot_each, total), bf16),
            pltpu.VMEM((head_each, payload), bf16),
        ),
        in_specs=[hbm_spec] * 6 + [vmem_spec] * 4,
        scratch_shapes=[
            pltpu.VMEM((seq_count, pos_local, features), bf16),
            pltpu.VMEM((features, latent), bf16),
            pltpu.VMEM((rope, features), bf16),
            pltpu.VMEM((width, heads, plain), bf16),
            pltpu.VMEM((width, heads, payload), bf16),
            pltpu.VMEM((seq_count * pos_local // ROW_CHUNKS, features), bf16),
            pltpu.VMEM((n, pos_local, width), bf16),
            pltpu.VMEM((n, prow, LANES), bf16),
            pltpu.VMEM((n, pos_local, width), bf16),
            pltpu.VMEM((n, prow, LANES), bf16),
            pltpu.VMEM((tp_count, head_each, 2 * LANES), f32),
            pltpu.VMEM((heads, 2 * LANES), f32),
            pltpu.VMEM((tp_count, heads, total), bf16),
            pltpu.VMEM((tp_count, head_each, payload), f32),
            pltpu.VMEM((tp_count, head_each, payload), f32),
            pltpu.VMEM((width * heads, width), bf16),
            pltpu.VMEM((total, n * prow), bf16),
            pltpu.VMEM((2, pos_local + 8, rope), f32),
            dma((seq_count + K_CHUNKS + 5,)),
            dma((2,)),
            dma((2,)),
            dma((tp_count - 1,)),
            dma((tp_count - 1,)),
            dma((tp_count - 1,)),
            dma((tp_count - 1,)),
            dma((tp_count - 1,)),
            dma((tp_count - 1,)),
        ],
        compiler_params=pltpu.CompilerParams(
            collective_id=0, has_side_effects=True, vmem_limit_bytes=VMEM_BYTES - held
        ),
    )(
        layer_input,
        narrowing_matrix,
        rotary_down.T,
        lookup_widening,
        payload_widening,
        table,
        input_gain.reshape(1, -1),
        summary_scaling.reshape(1, -1),
        query_nope[0],
        query_rotary[0],
    )
    results = (cache, rotary, read)
    cache, rotary, read = pl.pallas_call(
        write_out,
        out_shape=tuple(jax.ShapeDtypeStruct(r.shape, r.dtype) for r in results),
        in_specs=[vmem_spec] * 3,
        out_specs=(hbm_spec,) * 3,
        scratch_shapes=[dma((3,))],
        compiler_params=pltpu.CompilerParams(vmem_limit_bytes=1024 * 1024),
    )(*results)
    return (
        cache.reshape(1, total, width),
        rotary.T.reshape(1, total, rot_each),
        read.reshape(1, head_each, payload),
    )


def solution(mesh):
    return jax.shard_map(
        shards,
        mesh=mesh,
        in_specs=(
            P(None, ("sp", "tp"), None),
            P(),
            P(),
            P(),
            P(),
            P("tp", None, None),
            P("tp", None, None),
            P("sp", "tp", None),
            P("sp", "tp", None),
        ),
        out_specs=(P("sp", None, "tp"), P("sp", None, "tp"), P("sp", "tp", None)),
        check_vma=False,
    )
```

```python
import functools

import jax
import jax.numpy as jnp
import numpy as np
from jax import lax
from jax.experimental import pallas as pl
from jax.experimental.pallas import tpu as pltpu
from jax.sharding import PartitionSpec as P

QK_ROPE = 64
PLAIN_MATCH_SPAN = 128

norm_eps = 1e-06
rotary_base = 10000.0
LANES = 128
VMEM_BYTES = 67043328
ROW_CHUNKS = 2
K_CHUNKS = 4
MESH = pl.DeviceIdType.MESH
f32 = jnp.float32
bf16 = jnp.bfloat16


def rescaled_lines(vector):
    return vector * lax.rsqrt(jnp.mean(vector * vector, axis=-1, keepdims=True) + norm_eps)


def iota(shape, axis):
    return lax.broadcasted_iota(jnp.int32, shape, axis)


def quot(values, by):
    if by & (by - 1):
        return values // by
    return lax.shift_right_logical(values, jnp.int32(by.bit_length() - 1))


def rest(values, by):
    if by & (by - 1):
        return values % by
    return values & jnp.int32(by - 1)


def one_hot(cond):
    return jnp.where(cond, 1.0, 0.0).astype(bf16)


def dot(a, b):
    return jnp.dot(a, b, preferred_element_type=f32)


def dot_t(a, b):
    return lax.dot_general(a, b, (((1,), (1,)), ((), ())), preferred_element_type=f32)


def kernel(
    dims,
    x_hbm,
    w_hbm,
    wr_hbm,
    lw_hbm,
    pw_hbm,
    table_hbm,
    gain_ref,
    sgain_ref,
    q_ref,
    qr_ref,
    cache_out,
    rotary_out,
    read_out,
    x_ref,
    w_ref,
    wr_ref,
    lw_ref,
    pw_ref,
    xn_ref,
    stage,
    rstage,
    lat_recv,
    rot_recv,
    q_recv,
    q_all,
    s_recv,
    v_send,
    v_recv,
    spread,
    unpack,
    table_ref,
    load_sem,
    lat_sem,
    rot_sem,
    q_send_sem,
    q_recv_sem,
    s_send_sem,
    s_recv_sem,
    v_send_sem,
    v_recv_sem,
):
    sp_count, tp_count = dims
    n = sp_count * tp_count
    seq_count, pos_local, features = x_ref.shape
    latent = w_ref.shape[1]
    rope = wr_ref.shape[0]
    width = latent // tp_count
    rot_each = rope // tp_count
    packs = LANES // rot_each
    prow = pos_local // packs
    head_each, plain = q_ref.shape
    heads = head_each * tp_count
    total = n * pos_local
    my_sp = lax.axis_index("sp")
    my_tp = lax.axis_index("tp")
    me = my_sp * tp_count + my_tp

    loads = {}

    def load(key, index, src, dst):
        copy = pltpu.make_async_copy(src, dst, load_sem.at[index])
        copy.start()
        loads[key] = copy

    kdepth = features // K_CHUNKS
    half_sp = sp_count // 2
    my_half = lax.div(my_sp, half_sp)
    in_half = lax.rem(my_sp, half_sp)

    def target(order):
        return lax.rem(my_sp + 1 + order, sp_count)

    for j in range(seq_count):
        load(("x", j), j, x_hbm.at[target(j)], x_ref.at[j])
    for k in range(K_CHUNKS):
        rows = pl.ds(k * kdepth, kdepth)
        load(("w", k), seq_count + k, w_hbm.at[rows], w_ref.at[rows])
    base = seq_count + K_CHUNKS
    load("wr", base, wr_hbm, wr_ref)
    load("lw", base + 1, lw_hbm, lw_ref)
    load("pw", base + 2, pw_hbm, pw_ref)
    load(
        "table",
        base + 3,
        table_hbm.at[:, pl.ds(me * pos_local, pos_local)],
        table_ref.at[:, pl.ds(0, pos_local)],
    )
    load(
        "last",
        base + 4,
        table_hbm.at[:, pl.ds(total, 8)],
        table_ref.at[:, pl.ds(pos_local, 8)],
    )

    barrier = pltpu.get_barrier_semaphore()

    def greet(i, carry):
        other = lax.rem(me + 1 + i, n)
        pl.semaphore_signal(
            barrier,
            inc=1,
            device_id=(lax.div(other, tp_count), lax.rem(other, tp_count)),
            device_id_type=MESH,
        )
        return carry

    lax.fori_loop(0, n - 1, greet, 0)

    q_recv[my_tp] = jnp.zeros(q_recv.shape[1:], f32)
    q_recv[my_tp, :, :plain] = q_ref[...].astype(f32)
    q_recv[my_tp, :, plain : plain + rope] = qr_ref[...].astype(f32)

    half = rope // 2
    row_r, col_r = iota((rope, rope), 0), iota((rope, rope), 1)
    swap = (
        jnp.where((row_r == col_r + half), -1.0, 0.0)
        + jnp.where((row_r + half == col_r), 1.0, 0.0)
    ).astype(bf16)
    wide = (rope, tp_count * LANES)
    tile = one_hot(
        iota(wide, 0)
        == quot(iota(wide, 1), LANES) * rot_each + rest(iota(wide, 1), rot_each)
    )

    pairs = []

    def remote(src, dst, send, recv, sp, tp):
        copy = pltpu.make_async_remote_copy(
            src_ref=src,
            dst_ref=dst,
            send_sem=send,
            recv_sem=recv,
            device_id=(sp, tp),
            device_id_type=MESH,
        )
        copy.start()
        return copy

    chunk_seq = seq_count // ROW_CHUNKS
    chunk = chunk_seq * pos_local
    pick_shape = (chunk_seq * prow, chunk)
    pick_row, pick_col = iota(pick_shape, 0), iota(pick_shape, 1)
    pick = one_hot(
        (quot(pick_row, prow) == quot(pick_col, pos_local))
        & (rest(pick_row, prow) == rest(pick_col, prow))
    )
    mask_shape = (chunk, tp_count * LANES)
    keep = quot(rest(iota(mask_shape, 1), LANES), rot_each) == quot(
        rest(iota(mask_shape, 0), pos_local), prow
    )

    for c in range(ROW_CHUNKS):
        for j in range(chunk_seq):
            at = c * chunk_seq + j
            loads[("x", at)].wait()
            rows = rescaled_lines(x_ref[at].astype(f32)) * gain_ref[...]
            xn_ref[pl.ds(j * pos_local, pos_local), :] = rows.astype(bf16)
        acc = None
        for k in range(K_CHUNKS):
            if c == 0:
                loads[("w", k)].wait()
            part = dot(
                xn_ref[:, k * kdepth : (k + 1) * kdepth],
                w_ref[k * kdepth : (k + 1) * kdepth, :],
            )
            acc = part if acc is None else acc + part
        if c == 0:
            loads["wr"].wait()
            loads["table"].wait()
            loads["last"].wait()
        cos = table_ref[0, :pos_local, :]
        sin = table_ref[1, :pos_local, :]
        rot = dot_t(xn_ref[...], wr_ref[...]).astype(bf16)
        hidden = rescaled_lines(acc.astype(bf16).astype(f32)) * sgain_ref[...]
        swapped = dot(rot, swap)
        turned = (
            rot.astype(f32).reshape(chunk_seq, pos_local, rope) * cos[None]
            + swapped.reshape(chunk_seq, pos_local, rope) * sin[None]
        ).reshape(chunk, rope)
        copies = dot(turned.astype(bf16), tile)
        packed = dot(pick, jnp.where(keep, copies, 0.0).astype(bf16))
        for j in range(chunk_seq):
            for t in range(tp_count):
                at = (c * chunk_seq + j) * tp_count + t
                stage[at] = hidden[
                    j * pos_local : (j + 1) * pos_local, t * width : (t + 1) * width
                ].astype(bf16)
                rstage[at] = packed[
                    j * prow : (j + 1) * prow, t * LANES : (t + 1) * LANES
                ].astype(bf16)
        if c == 0:
            pl.semaphore_wait(barrier, n - 1)
            for k in range(tp_count - 1):
                peer = lax.rem(my_tp + 1 + k, tp_count)
                pairs.append(
                    remote(
                        q_recv.at[my_tp],
                        q_recv.at[my_tp],
                        q_send_sem.at[k],
                        q_recv_sem.at[k],
                        my_sp,
                        peer,
                    )
                )
        for j in range(chunk_seq):
            order = c * chunk_seq + j
            to_sp = target(order)
            for k in range(tp_count):
                to_tp = lax.rem(my_tp + 1 + k, tp_count)
                at = order * tp_count + to_tp
                if order == seq_count - 1 and k == tp_count - 1:
                    lat_recv[me] = stage[at]
                    rot_recv[me] = rstage[at]
                else:
                    remote(
                        rstage.at[at], rot_recv.at[me], rot_sem.at[0], rot_sem.at[1], to_sp, to_tp
                    )
                    remote(
                        stage.at[at], lat_recv.at[me], lat_sem.at[0], lat_sem.at[1], to_sp, to_tp
                    )

    spread_shape = spread.shape
    spread[...] = one_hot(quot(iota(spread_shape, 0), heads) == iota(spread_shape, 1))
    own_shape = (heads, width * heads)
    own_head = iota(own_shape, 0) == rest(iota(own_shape, 1), heads)
    un_shape = unpack.shape
    un_row, un_col = iota(un_shape, 0), iota(un_shape, 1)
    unpack[...] = one_hot(
        (quot(un_row, pos_local) == quot(un_col, prow))
        & (rest(un_row, prow) == rest(un_col, prow))
    )
    rkeep_shape = (total, LANES)
    rkeep = quot(iota(rkeep_shape, 1), rot_each) == quot(
        rest(iota(rkeep_shape, 0), pos_local), prow
    )
    narrow = (rot_each, LANES)
    fold = one_hot(rest(iota(narrow, 1), rot_each) == iota(narrow, 0))

    for copy in pairs:
        copy.wait()
    for t in range(tp_count):
        q_all[t * head_each : (t + 1) * head_each, :] = q_recv[t]
    queries = q_all[:, :plain].astype(bf16)
    q_rot = q_all[:, plain : plain + rope]
    qcos = table_ref[0, pos_local : pos_local + 1, :]
    qsin = table_ref[1, pos_local : pos_local + 1, :]
    q_turned = (q_rot * qcos + dot(q_rot.astype(bf16), swap) * qsin).astype(bf16)
    share = (rope, rot_each)
    mine = one_hot(iota(share, 0) == iota(share, 1) + my_tp * rot_each)
    q_mine = dot(q_turned, mine).astype(bf16)
    loads["lw"].wait()
    lookup = lw_ref[...].reshape(width * heads, plain)
    every = dot_t(queries, lookup)
    absorbed = dot(jnp.where(own_head, every, 0.0).astype(bf16), spread[...]).astype(bf16)

    pltpu.make_async_copy(
        rot_recv.at[pl.ds(0, n - 1)], rot_recv.at[pl.ds(0, n - 1)], rot_sem.at[1]
    ).wait()
    rot_rows = rot_recv[...].astype(f32).reshape(n * prow, LANES).astype(bf16)
    rot_wide = jnp.where(rkeep, dot(unpack[...], rot_rows), 0.0).astype(bf16)
    rot_cache = dot_t(fold, rot_wide).astype(bf16)
    rotary_out[...] = rot_cache
    rot_part = dot(q_mine, rot_cache)

    pltpu.make_async_copy(
        lat_recv.at[pl.ds(0, n - 1)], lat_recv.at[pl.ds(0, n - 1)], lat_sem.at[1]
    ).wait()
    cache = lat_recv[...].reshape(total, width)
    score_scale = (PLAIN_MATCH_SPAN + QK_ROPE) ** (-0.5)
    s_recv[my_tp] = ((dot_t(absorbed, cache) + rot_part) * score_scale).astype(bf16)
    pairs = []
    for k in range(tp_count - 1):
        peer = lax.rem(my_tp + 1 + k, tp_count)
        pairs.append(
            remote(
                s_recv.at[my_tp],
                s_recv.at[my_tp],
                s_send_sem.at[k],
                s_recv_sem.at[k],
                my_sp,
                peer,
            )
        )
    loads["pw"].wait()
    for copy in pairs:
        copy.wait()
    scores = s_recv[0].astype(f32)
    for t in range(1, tp_count):
        scores = scores + s_recv[t].astype(f32)
    top = jnp.max(scores, axis=-1, keepdims=True)
    weights = jnp.exp(scores - top)
    attention = (weights / jnp.sum(weights, axis=-1, keepdims=True)).astype(bf16)
    context = dot(attention, cache).astype(bf16)
    laid = jnp.where(own_head, dot_t(context, spread[...]), 0.0).astype(bf16)
    payload = pw_ref[...].reshape(width * heads, pw_ref.shape[2])
    values = dot(laid, payload)
    for t in range(tp_count):
        v_send[t] = values[t * head_each : (t + 1) * head_each, :]
    v_recv[my_tp] = v_send[my_tp]
    pairs = []
    for k in range(tp_count - 1):
        peer = lax.rem(my_tp + 1 + k, tp_count)
        pairs.append(
            remote(
                v_send.at[peer],
                v_recv.at[my_tp],
                v_send_sem.at[k],
                v_recv_sem.at[k],
                my_sp,
                peer,
            )
        )
    pltpu.make_async_copy(
        rstage.at[pl.ds(0, n - 1)], rstage.at[pl.ds(0, n - 1)], rot_sem.at[0]
    ).wait()
    pltpu.make_async_copy(
        stage.at[pl.ds(0, n - 1)], stage.at[pl.ds(0, n - 1)], lat_sem.at[0]
    ).wait()
    cache_out[...] = lat_recv[...]
    for copy in pairs:
        copy.wait()
    summed = v_recv[0]
    for t in range(1, tp_count):
        summed = summed + v_recv[t]
    read_out[...] = rescaled_lines(summed).astype(bf16)


def rotary_table(total, rope):
    half = rope // 2
    frequency = 1.0 / rotary_base ** (np.arange(half) * 2.0 / rope)
    frequency = np.concatenate([frequency, frequency]).astype(np.float32)
    spots = np.minimum(np.arange(total + 8), total).astype(np.float32)
    angles = (spots[:, None] * frequency[None, :]).astype(np.float64)
    return np.stack([np.cos(angles), np.sin(angles)]).astype(np.float32)


def write_out(cache_ref, rotary_ref, read_ref, cache_hbm, rotary_hbm, read_hbm, sems):
    copies = [
        pltpu.make_async_copy(src, dst, sems.at[i])
        for i, (src, dst) in enumerate(
            ((cache_ref, cache_hbm), (rotary_ref, rotary_hbm), (read_ref, read_hbm))
        )
    ]
    for copy in copies:
        copy.start()
    for copy in copies:
        copy.wait()


def shards(
    layer_input,
    input_gain,
    narrowing_matrix,
    rotary_down,
    summary_scaling,
    lookup_widening,
    payload_widening,
    query_nope,
    query_rotary,
):
    seq_count, pos_local, features = layer_input.shape
    sp_count = lax.axis_size("sp")
    tp_count = lax.axis_size("tp")
    n = sp_count * tp_count
    assert seq_count == sp_count
    latent = narrowing_matrix.shape[1]
    rope = rotary_down.shape[1]
    width, heads, plain = lookup_widening.shape
    payload = payload_widening.shape[2]
    head_each = query_nope.shape[1]
    rot_each = rope // tp_count
    prow = pos_local * rot_each // LANES
    total = n * pos_local
    table = jnp.asarray(rotary_table(total, rope))
    held = 2 * total * (max(width, LANES) + max(rot_each, 16)) + 52 * 1024
    hbm_spec = pl.BlockSpec(memory_space=pltpu.HBM)
    vmem_spec = pl.BlockSpec(memory_space=pltpu.VMEM)
    dma = pltpu.SemaphoreType.DMA
    cache, rotary, read = pl.pallas_call(
        functools.partial(kernel, (sp_count, tp_count)),
        out_shape=(
            pltpu.VMEM((n, pos_local, width), bf16),
            pltpu.VMEM((rot_each, total), bf16),
            pltpu.VMEM((head_each, payload), bf16),
        ),
        in_specs=[hbm_spec] * 6 + [vmem_spec] * 4,
        scratch_shapes=[
            pltpu.VMEM((seq_count, pos_local, features), bf16),
            pltpu.VMEM((features, latent), bf16),
            pltpu.VMEM((rope, features), bf16),
            pltpu.VMEM((width, heads, plain), bf16),
            pltpu.VMEM((width, heads, payload), bf16),
            pltpu.VMEM((seq_count * pos_local // ROW_CHUNKS, features), bf16),
            pltpu.VMEM((n, pos_local, width), bf16),
            pltpu.VMEM((n, prow, LANES), bf16),
            pltpu.VMEM((n, pos_local, width), bf16),
            pltpu.VMEM((n, prow, LANES), bf16),
            pltpu.VMEM((tp_count, head_each, 2 * LANES), f32),
            pltpu.VMEM((heads, 2 * LANES), f32),
            pltpu.VMEM((tp_count, heads, total), bf16),
            pltpu.VMEM((tp_count, head_each, payload), f32),
            pltpu.VMEM((tp_count, head_each, payload), f32),
            pltpu.VMEM((width * heads, width), bf16),
            pltpu.VMEM((total, n * prow), bf16),
            pltpu.VMEM((2, pos_local + 8, rope), f32),
            dma((seq_count + K_CHUNKS + 5,)),
            dma((2,)),
            dma((2,)),
            dma((tp_count - 1,)),
            dma((tp_count - 1,)),
            dma((tp_count - 1,)),
            dma((tp_count - 1,)),
            dma((tp_count - 1,)),
            dma((tp_count - 1,)),
        ],
        compiler_params=pltpu.CompilerParams(
            collective_id=0, has_side_effects=True, vmem_limit_bytes=VMEM_BYTES - held
        ),
    )(
        layer_input,
        narrowing_matrix,
        rotary_down.T,
        lookup_widening,
        payload_widening,
        table,
        input_gain.reshape(1, -1),
        summary_scaling.reshape(1, -1),
        query_nope[0],
        query_rotary[0],
    )
    results = (cache, rotary, read)
    cache, rotary, read = pl.pallas_call(
        write_out,
        out_shape=tuple(jax.ShapeDtypeStruct(r.shape, r.dtype) for r in results),
        in_specs=[vmem_spec] * 3,
        out_specs=(hbm_spec,) * 3,
        scratch_shapes=[dma((3,))],
        compiler_params=pltpu.CompilerParams(vmem_limit_bytes=1024 * 1024),
    )(*results)
    return (
        cache.reshape(1, total, width),
        rotary.T.reshape(1, total, rot_each),
        read.reshape(1, head_each, payload),
    )


def solution(mesh):
    return jax.shard_map(
        shards,
        mesh=mesh,
        in_specs=(
            P(None, ("sp", "tp"), None),
            P(),
            P(),
            P(),
            P(),
            P("tp", None, None),
            P("tp", None, None),
            P("sp", "tp", None),
            P("sp", "tp", None),
        ),
        out_specs=(P("sp", None, "tp"), P("sp", None, "tp"), P("sp", "tp", None)),
        check_vma=False,
    )
```

```python
import functools

import jax
import jax.numpy as jnp
import numpy as np
from jax import lax
from jax.experimental import pallas as pl
from jax.experimental.pallas import tpu as pltpu
from jax.sharding import PartitionSpec as P

QK_ROPE = 64
PLAIN_MATCH_SPAN = 128

norm_eps = 1e-06
rotary_base = 10000.0
LANES = 128
VMEM_BYTES = 67043328
ROW_CHUNKS = 2
K_CHUNKS = 4
MESH = pl.DeviceIdType.MESH
f32 = jnp.float32
bf16 = jnp.bfloat16


def rescaled_lines(vector):
    return vector * lax.rsqrt(jnp.mean(vector * vector, axis=-1, keepdims=True) + norm_eps)


def iota(shape, axis):
    return lax.broadcasted_iota(jnp.int32, shape, axis)


def quot(values, by):
    if by & (by - 1):
        return values // by
    return lax.shift_right_logical(values, jnp.int32(by.bit_length() - 1))


def rest(values, by):
    if by & (by - 1):
        return values % by
    return values & jnp.int32(by - 1)


def one_hot(cond):
    return jnp.where(cond, 1.0, 0.0).astype(bf16)


def dot(a, b):
    return jnp.dot(a, b, preferred_element_type=f32)


def dot_t(a, b):
    return lax.dot_general(a, b, (((1,), (1,)), ((), ())), preferred_element_type=f32)


def kernel(
    dims,
    x_hbm,
    w_hbm,
    wr_hbm,
    lw_hbm,
    pw_hbm,
    table_hbm,
    gain_ref,
    sgain_ref,
    q_ref,
    qr_ref,
    cache_out,
    rotary_out,
    read_out,
    x_ref,
    w_ref,
    wr_ref,
    lw_ref,
    pw_ref,
    xn_ref,
    stage,
    rstage,
    lat_recv,
    rot_recv,
    q_recv,
    q_all,
    s_recv,
    v_send,
    v_recv,
    spread,
    unpack,
    table_ref,
    load_sem,
    lat_sem,
    rot_sem,
    q_send_sem,
    q_recv_sem,
    s_send_sem,
    s_recv_sem,
    v_send_sem,
    v_recv_sem,
):
    sp_count, tp_count = dims
    n = sp_count * tp_count
    seq_count, pos_local, features = x_ref.shape
    latent = w_ref.shape[1]
    rope = wr_ref.shape[0]
    width = latent // tp_count
    rot_each = rope // tp_count
    packs = LANES // rot_each
    prow = pos_local // packs
    head_each, plain = q_ref.shape
    heads = head_each * tp_count
    total = n * pos_local
    my_sp = lax.axis_index("sp")
    my_tp = lax.axis_index("tp")
    me = my_sp * tp_count + my_tp

    loads = {}

    def load(key, index, src, dst):
        copy = pltpu.make_async_copy(src, dst, load_sem.at[index])
        copy.start()
        loads[key] = copy

    kdepth = features // K_CHUNKS
    half_sp = sp_count // 2
    my_half = lax.div(my_sp, half_sp)
    in_half = lax.rem(my_sp, half_sp)

    def target(order):
        return lax.rem(my_sp + 1 + order, sp_count)

    for j in range(seq_count):
        load(("x", j), j, x_hbm.at[target(j)], x_ref.at[j])
    for k in range(K_CHUNKS):
        rows = pl.ds(k * kdepth, kdepth)
        load(("w", k), seq_count + k, w_hbm.at[rows], w_ref.at[rows])
    base = seq_count + K_CHUNKS
    load("wr", base, wr_hbm, wr_ref)
    load("lw", base + 1, lw_hbm, lw_ref)
    load("pw", base + 2, pw_hbm, pw_ref)
    load(
        "table",
        base + 3,
        table_hbm.at[:, pl.ds(me * pos_local, pos_local)],
        table_ref.at[:, pl.ds(0, pos_local)],
    )
    load(
        "last",
        base + 4,
        table_hbm.at[:, pl.ds(total, 8)],
        table_ref.at[:, pl.ds(pos_local, 8)],
    )

    barrier = pltpu.get_barrier_semaphore()

    def greet(i, carry):
        other = lax.rem(me + 1 + i, n)
        pl.semaphore_signal(
            barrier,
            inc=1,
            device_id=(lax.div(other, tp_count), lax.rem(other, tp_count)),
            device_id_type=MESH,
        )
        return carry

    lax.fori_loop(0, n - 1, greet, 0)

    q_recv[my_tp] = jnp.zeros(q_recv.shape[1:], f32)
    q_recv[my_tp, :, :plain] = q_ref[...].astype(f32)
    q_recv[my_tp, :, plain : plain + rope] = qr_ref[...].astype(f32)

    half = rope // 2
    row_r, col_r = iota((rope, rope), 0), iota((rope, rope), 1)
    swap = (
        jnp.where((row_r == col_r + half), -1.0, 0.0)
        + jnp.where((row_r + half == col_r), 1.0, 0.0)
    ).astype(bf16)
    wide = (rope, tp_count * LANES)
    tile = one_hot(
        iota(wide, 0)
        == quot(iota(wide, 1), LANES) * rot_each + rest(iota(wide, 1), rot_each)
    )

    pairs = []

    def remote(src, dst, send, recv, sp, tp):
        copy = pltpu.make_async_remote_copy(
            src_ref=src,
            dst_ref=dst,
            send_sem=send,
            recv_sem=recv,
            device_id=(sp, tp),
            device_id_type=MESH,
        )
        copy.start()
        return copy

    chunk_seq = seq_count // ROW_CHUNKS
    chunk = chunk_seq * pos_local
    pick_shape = (chunk_seq * prow, chunk)
    pick_row, pick_col = iota(pick_shape, 0), iota(pick_shape, 1)
    pick = one_hot(
        (quot(pick_row, prow) == quot(pick_col, pos_local))
        & (rest(pick_row, prow) == rest(pick_col, prow))
    )
    mask_shape = (chunk, tp_count * LANES)
    keep = quot(rest(iota(mask_shape, 1), LANES), rot_each) == quot(
        rest(iota(mask_shape, 0), pos_local), prow
    )

    for c in range(ROW_CHUNKS):
        for j in range(chunk_seq):
            at = c * chunk_seq + j
            loads[("x", at)].wait()
            rows = rescaled_lines(x_ref[at].astype(f32)) * gain_ref[...]
            xn_ref[pl.ds(j * pos_local, pos_local), :] = rows.astype(bf16)
        acc = None
        for k in range(K_CHUNKS):
            if c == 0:
                loads[("w", k)].wait()
            part = dot(
                xn_ref[:, k * kdepth : (k + 1) * kdepth],
                w_ref[k * kdepth : (k + 1) * kdepth, :],
            )
            acc = part if acc is None else acc + part
        if c == 0:
            loads["wr"].wait()
            loads["table"].wait()
            loads["last"].wait()
        cos = table_ref[0, :pos_local, :]
        sin = table_ref[1, :pos_local, :]
        rot = dot_t(xn_ref[...], wr_ref[...]).astype(bf16)
        hidden = rescaled_lines(acc.astype(bf16).astype(f32)) * sgain_ref[...]
        swapped = dot(rot, swap)
        turned = (
            rot.astype(f32).reshape(chunk_seq, pos_local, rope) * cos[None]
            + swapped.reshape(chunk_seq, pos_local, rope) * sin[None]
        ).reshape(chunk, rope)
        copies = dot(turned.astype(bf16), tile)
        packed = dot(pick, jnp.where(keep, copies, 0.0).astype(bf16))
        for j in range(chunk_seq):
            for t in range(tp_count):
                at = (c * chunk_seq + j) * tp_count + t
                stage[at] = hidden[
                    j * pos_local : (j + 1) * pos_local, t * width : (t + 1) * width
                ].astype(bf16)
                rstage[at] = packed[
                    j * prow : (j + 1) * prow, t * LANES : (t + 1) * LANES
                ].astype(bf16)
        if c == 0:
            pl.semaphore_wait(barrier, n - 1)
            for k in range(tp_count - 1):
                peer = lax.rem(my_tp + 1 + k, tp_count)
                pairs.append(
                    remote(
                        q_recv.at[my_tp],
                        q_recv.at[my_tp],
                        q_send_sem.at[k],
                        q_recv_sem.at[k],
                        my_sp,
                        peer,
                    )
                )
        for j in range(chunk_seq):
            order = c * chunk_seq + j
            to_sp = target(order)
            for k in range(tp_count):
                to_tp = lax.rem(my_tp + tp_count - 1 - k, tp_count)
                at = order * tp_count + to_tp
                if order == seq_count - 1 and k == tp_count - 1:
                    lat_recv[me] = stage[at]
                    rot_recv[me] = rstage[at]
                else:
                    remote(
                        rstage.at[at], rot_recv.at[me], rot_sem.at[0], rot_sem.at[1], to_sp, to_tp
                    )
                    remote(
                        stage.at[at], lat_recv.at[me], lat_sem.at[0], lat_sem.at[1], to_sp, to_tp
                    )

    spread_shape = spread.shape
    spread[...] = one_hot(quot(iota(spread_shape, 0), heads) == iota(spread_shape, 1))
    own_shape = (heads, width * heads)
    own_head = iota(own_shape, 0) == rest(iota(own_shape, 1), heads)
    un_shape = unpack.shape
    un_row, un_col = iota(un_shape, 0), iota(un_shape, 1)
    unpack[...] = one_hot(
        (quot(un_row, pos_local) == quot(un_col, prow))
        & (rest(un_row, prow) == rest(un_col, prow))
    )
    rkeep_shape = (total, LANES)
    rkeep = quot(iota(rkeep_shape, 1), rot_each) == quot(
        rest(iota(rkeep_shape, 0), pos_local), prow
    )
    narrow = (rot_each, LANES)
    fold = one_hot(rest(iota(narrow, 1), rot_each) == iota(narrow, 0))

    for copy in pairs:
        copy.wait()
    for t in range(tp_count):
        q_all[t * head_each : (t + 1) * head_each, :] = q_recv[t]
    queries = q_all[:, :plain].astype(bf16)
    q_rot = q_all[:, plain : plain + rope]
    qcos = table_ref[0, pos_local : pos_local + 1, :]
    qsin = table_ref[1, pos_local : pos_local + 1, :]
    q_turned = (q_rot * qcos + dot(q_rot.astype(bf16), swap) * qsin).astype(bf16)
    share = (rope, rot_each)
    mine = one_hot(iota(share, 0) == iota(share, 1) + my_tp * rot_each)
    q_mine = dot(q_turned, mine).astype(bf16)
    loads["lw"].wait()
    lookup = lw_ref[...].reshape(width * heads, plain)
    every = dot_t(queries, lookup)
    absorbed = dot(jnp.where(own_head, every, 0.0).astype(bf16), spread[...]).astype(bf16)

    pltpu.make_async_copy(
        rot_recv.at[pl.ds(0, n - 1)], rot_recv.at[pl.ds(0, n - 1)], rot_sem.at[1]
    ).wait()
    rot_rows = rot_recv[...].astype(f32).reshape(n * prow, LANES).astype(bf16)
    rot_wide = jnp.where(rkeep, dot(unpack[...], rot_rows), 0.0).astype(bf16)
    rot_cache = dot_t(fold, rot_wide).astype(bf16)
    rotary_out[...] = rot_cache
    rot_part = dot(q_mine, rot_cache)

    pltpu.make_async_copy(
        lat_recv.at[pl.ds(0, n - 1)], lat_recv.at[pl.ds(0, n - 1)], lat_sem.at[1]
    ).wait()
    cache = lat_recv[...].reshape(total, width)
    score_scale = (PLAIN_MATCH_SPAN + QK_ROPE) ** (-0.5)
    s_recv[my_tp] = ((dot_t(absorbed, cache) + rot_part) * score_scale).astype(bf16)
    pairs = []
    for k in range(tp_count - 1):
        peer = lax.rem(my_tp + 1 + k, tp_count)
        pairs.append(
            remote(
                s_recv.at[my_tp],
                s_recv.at[my_tp],
                s_send_sem.at[k],
                s_recv_sem.at[k],
                my_sp,
                peer,
            )
        )
    loads["pw"].wait()
    for copy in pairs:
        copy.wait()
    scores = s_recv[0].astype(f32)
    for t in range(1, tp_count):
        scores = scores + s_recv[t].astype(f32)
    top = jnp.max(scores, axis=-1, keepdims=True)
    weights = jnp.exp(scores - top)
    attention = (weights / jnp.sum(weights, axis=-1, keepdims=True)).astype(bf16)
    context = dot(attention, cache).astype(bf16)
    laid = jnp.where(own_head, dot_t(context, spread[...]), 0.0).astype(bf16)
    payload = pw_ref[...].reshape(width * heads, pw_ref.shape[2])
    values = dot(laid, payload)
    for t in range(tp_count):
        v_send[t] = values[t * head_each : (t + 1) * head_each, :]
    v_recv[my_tp] = v_send[my_tp]
    pairs = []
    for k in range(tp_count - 1):
        peer = lax.rem(my_tp + 1 + k, tp_count)
        pairs.append(
            remote(
                v_send.at[peer],
                v_recv.at[my_tp],
                v_send_sem.at[k],
                v_recv_sem.at[k],
                my_sp,
                peer,
            )
        )
    pltpu.make_async_copy(
        rstage.at[pl.ds(0, n - 1)], rstage.at[pl.ds(0, n - 1)], rot_sem.at[0]
    ).wait()
    pltpu.make_async_copy(
        stage.at[pl.ds(0, n - 1)], stage.at[pl.ds(0, n - 1)], lat_sem.at[0]
    ).wait()
    cache_out[...] = lat_recv[...]
    for copy in pairs:
        copy.wait()
    summed = v_recv[0]
    for t in range(1, tp_count):
        summed = summed + v_recv[t]
    read_out[...] = rescaled_lines(summed).astype(bf16)


def rotary_table(total, rope):
    half = rope // 2
    frequency = 1.0 / rotary_base ** (np.arange(half) * 2.0 / rope)
    frequency = np.concatenate([frequency, frequency]).astype(np.float32)
    spots = np.minimum(np.arange(total + 8), total).astype(np.float32)
    angles = (spots[:, None] * frequency[None, :]).astype(np.float64)
    return np.stack([np.cos(angles), np.sin(angles)]).astype(np.float32)


def write_out(cache_ref, rotary_ref, read_ref, cache_hbm, rotary_hbm, read_hbm, sems):
    copies = [
        pltpu.make_async_copy(src, dst, sems.at[i])
        for i, (src, dst) in enumerate(
            ((cache_ref, cache_hbm), (rotary_ref, rotary_hbm), (read_ref, read_hbm))
        )
    ]
    for copy in copies:
        copy.start()
    for copy in copies:
        copy.wait()


def shards(
    layer_input,
    input_gain,
    narrowing_matrix,
    rotary_down,
    summary_scaling,
    lookup_widening,
    payload_widening,
    query_nope,
    query_rotary,
):
    seq_count, pos_local, features = layer_input.shape
    sp_count = lax.axis_size("sp")
    tp_count = lax.axis_size("tp")
    n = sp_count * tp_count
    assert seq_count == sp_count
    latent = narrowing_matrix.shape[1]
    rope = rotary_down.shape[1]
    width, heads, plain = lookup_widening.shape
    payload = payload_widening.shape[2]
    head_each = query_nope.shape[1]
    rot_each = rope // tp_count
    prow = pos_local * rot_each // LANES
    total = n * pos_local
    table = jnp.asarray(rotary_table(total, rope))
    held = 2 * total * (max(width, LANES) + max(rot_each, 16)) + 52 * 1024
    hbm_spec = pl.BlockSpec(memory_space=pltpu.HBM)
    vmem_spec = pl.BlockSpec(memory_space=pltpu.VMEM)
    dma = pltpu.SemaphoreType.DMA
    cache, rotary, read = pl.pallas_call(
        functools.partial(kernel, (sp_count, tp_count)),
        out_shape=(
            pltpu.VMEM((n, pos_local, width), bf16),
            pltpu.VMEM((rot_each, total), bf16),
            pltpu.VMEM((head_each, payload), bf16),
        ),
        in_specs=[hbm_spec] * 6 + [vmem_spec] * 4,
        scratch_shapes=[
            pltpu.VMEM((seq_count, pos_local, features), bf16),
            pltpu.VMEM((features, latent), bf16),
            pltpu.VMEM((rope, features), bf16),
            pltpu.VMEM((width, heads, plain), bf16),
            pltpu.VMEM((width, heads, payload), bf16),
            pltpu.VMEM((seq_count * pos_local // ROW_CHUNKS, features), bf16),
            pltpu.VMEM((n, pos_local, width), bf16),
            pltpu.VMEM((n, prow, LANES), bf16),
            pltpu.VMEM((n, pos_local, width), bf16),
            pltpu.VMEM((n, prow, LANES), bf16),
            pltpu.VMEM((tp_count, head_each, 2 * LANES), f32),
            pltpu.VMEM((heads, 2 * LANES), f32),
            pltpu.VMEM((tp_count, heads, total), bf16),
            pltpu.VMEM((tp_count, head_each, payload), f32),
            pltpu.VMEM((tp_count, head_each, payload), f32),
            pltpu.VMEM((width * heads, width), bf16),
            pltpu.VMEM((total, n * prow), bf16),
            pltpu.VMEM((2, pos_local + 8, rope), f32),
            dma((seq_count + K_CHUNKS + 5,)),
            dma((2,)),
            dma((2,)),
            dma((tp_count - 1,)),
            dma((tp_count - 1,)),
            dma((tp_count - 1,)),
            dma((tp_count - 1,)),
            dma((tp_count - 1,)),
            dma((tp_count - 1,)),
        ],
        compiler_params=pltpu.CompilerParams(
            collective_id=0, has_side_effects=True, vmem_limit_bytes=VMEM_BYTES - held
        ),
    )(
        layer_input,
        narrowing_matrix,
        rotary_down.T,
        lookup_widening,
        payload_widening,
        table,
        input_gain.reshape(1, -1),
        summary_scaling.reshape(1, -1),
        query_nope[0],
        query_rotary[0],
    )
    results = (cache, rotary, read)
    cache, rotary, read = pl.pallas_call(
        write_out,
        out_shape=tuple(jax.ShapeDtypeStruct(r.shape, r.dtype) for r in results),
        in_specs=[vmem_spec] * 3,
        out_specs=(hbm_spec,) * 3,
        scratch_shapes=[dma((3,))],
        compiler_params=pltpu.CompilerParams(vmem_limit_bytes=1024 * 1024),
    )(*results)
    return (
        cache.reshape(1, total, width),
        rotary.T.reshape(1, total, rot_each),
        read.reshape(1, head_each, payload),
    )


def solution(mesh):
    return jax.shard_map(
        shards,
        mesh=mesh,
        in_specs=(
            P(None, ("sp", "tp"), None),
            P(),
            P(),
            P(),
            P(),
            P("tp", None, None),
            P("tp", None, None),
            P("sp", "tp", None),
            P("sp", "tp", None),
        ),
        out_specs=(P("sp", None, "tp"), P("sp", None, "tp"), P("sp", "tp", None)),
        check_vma=False,
    )
```
